256 devices in a mesh: fs: 32 (over z, x), tp: 8 (over y, core).
Axes of the slice: x: 4, y: 4, z: 8, core: 2. Of those that a mesh axis runs over, the one named last changes fastest.
Arguments:
- later_input: bfloat16 [32768, 2048], P(('fs', 'tp')), may hold values from -6 to 6
- saved_input: bfloat16 [32768, 2048], P(('fs', 'tp')), may hold values from -24 to 24
- cotangent: bfloat16 [32768, 3072], P('fs', 'tp'), may hold values from -6 to 6
- up_weight: bfloat16 [2048, 3072], P('fs', 'tp'), may hold values from -0.125 to 0.125
- gate_weight: bfloat16 [2048, 3072], P('fs', 'tp'), may hold values from -0.125 to 0.125
- up_taps: bfloat16 [3, 3072], replicated, may hold values from -3.5 to 3.5
- gate_taps: bfloat16 [3, 3072], replicated, may hold values from -3.5 to 3.5
- up_grad_sum: float32 [2048, 3072], P('fs', 'tp'), may hold values from -6 to 6
- gate_grad_sum: float32 [2048, 3072], P('fs', 'tp'), may hold values from -6 to 6
- up_taps_sum: float32 [3, 3072], replicated, may hold values from -6 to 6
- gate_taps_sum: float32 [3, 3072], replicated, may hold values from -6 to 6
Outputs:
- hidden: bfloat16 [32768, 3072], P('fs', 'tp')
- input_grad: bfloat16 [32768, 2048], P(('fs', 'tp'))
- new_up_sum: float32 [2048, 3072], P('fs', 'tp')
- new_gate_sum: float32 [2048, 3072], P('fs', 'tp')
- new_up_taps_sum: float32 [3, 3072], replicated
- new_gate_taps_sum: float32 [3, 3072], replicated
The draws below stay inside these ranges and needn't reach their ends.
All inputs are finite; a program needn't handle non-finite values.
Results may differ from the reference program's by a relative error of at most 0.018.
Values may be sent and summed in bfloat16 or wider, within the bound.
No kernel may reach another device: no remote copies, remote signals or barrier semaphores. Data moves between devices by JAX's collectives and lax.ppermute only.
A program may use at most 64 MiB of HBM per device.

```python
import jax
import jax.numpy as jnp
from jax import lax

D = 2048
FF = 3072
TOKENS = 32768
N_FS = 32
N_TP = 8


def raised(array, key, source, target, blocks, factor):
    def block_of(axis_at):
        return (jnp.arange(array.shape[axis_at]) // (array.shape[axis_at] // blocks)).reshape((-1,) + (1,) * (array.ndim - 1 - axis_at))

    near = jax.random.permutation(key, blocks)[block_of(target)]
    other_side = (block_of(target) + blocks // 2) % blocks
    return jnp.where((block_of(source) == near) | (block_of(source) == other_side), factor * array, array)


def level_of(own_key, extent, shards, least, largest):
    loudness = 1.0
    for dim, shards_of in shards:
        steps = jax.random.uniform(jax.random.fold_in(jax.random.fold_in(own_key, 6), dim), (shards_of,), jnp.float32, least / len(shards), largest / len(shards))
        loudness = loudness * jnp.repeat(jnp.exp(steps), extent[dim] // shards_of).reshape((-1,) + (1,) * (len(extent) - 1 - dim))
    return loudness


def noise(rng, shape, deviation, limit, shards=(), dtype=jnp.bfloat16):
    result = deviation * jax.random.normal(rng, shape, jnp.float32)
    if shards:
        result = result * level_of(rng, shape, shards, -0.22, 0.18)
    return jnp.clip(result, -limit, limit).astype(dtype)


def noise_with(rng, extent, spread, reach, pieces, heavy, dtype=jnp.bfloat16):
    drawn = spread * jax.random.normal(rng, extent, jnp.float32)
    if pieces:
        drawn = drawn * level_of(rng, extent, pieces, -0.22, 0.18)
    return jnp.clip(raised(drawn, jax.random.fold_in(rng, 3), *heavy), -reach, reach).astype(dtype)


def setup_inputs(seed: int = 0) -> dict:
    splits = jax.random.split(jax.random.key(seed), 12)
    return {
        "later_input": noise(splits[0], (TOKENS, D), 1.0, 6.0, ((0, 256),)),
        "saved_input": noise_with(splits[1], (TOKENS, D), 1.0, 24.0, ((0, 256),), (0, 1, 256, 6.0)),
        "cotangent": noise_with(splits[2], (TOKENS, FF), 1.0, 6.0, ((0, 32), (1, 8)), (1, 0, 32, 2.75)),
        "up_weight": noise(splits[3], (D, FF), D ** -0.5, 0.125, ((0, 32), (1, 8))),
        "gate_weight": noise(splits[4], (D, FF), D ** -0.5, 0.125, ((0, 32), (1, 8))),
        "up_taps": noise(splits[5], (3, FF), 3 ** -0.5, 3.5),
        "gate_taps": noise(splits[6], (3, FF), 3 ** -0.5, 3.5),
        "up_grad_sum": noise(splits[7], (D, FF), 1.0, 6.0, ((0, 32), (1, 8)), jnp.float32),
        "gate_grad_sum": noise(splits[8], (D, FF), 1.0, 6.0, ((0, 32), (1, 8)), jnp.float32),
        "up_taps_sum": noise(splits[9], (3, FF), 1.0, 6.0, (), jnp.float32),
        "gate_taps_sum": noise(splits[10], (3, FF), 1.0, 6.0, (), jnp.float32),
    }


def delayed(values, steps):
    zeros = jnp.zeros_like(values[:steps])
    return jnp.concatenate([zeros, values[:-steps]], axis=0)

def advanced(values, steps):
    zeros = jnp.zeros_like(values[:steps])
    return jnp.concatenate([values[steps:], zeros], axis=0)

def depthwise(values, taps):
    return taps[2] * values + taps[1] * delayed(values, 1) + taps[0] * delayed(values, 2)

def depthwise_back(grads, taps):
    return taps[2] * grads + taps[1] * advanced(grads, 1) + taps[0] * advanced(grads, 2)

def taps_grad(grads, values):
    return jnp.stack([lax.optimization_barrier(jnp.sum(grads * delayed(values, 2), axis=0)), lax.optimization_barrier(jnp.sum(grads * delayed(values, 1), axis=0)), lax.optimization_barrier(jnp.sum(grads * values, axis=0))], axis=0)

def reference(later_input, saved_input, cotangent, up_weight, gate_weight, up_taps, gate_taps, up_grad_sum, gate_grad_sum, up_taps_sum, gate_taps_sum):
    tokens_all = later_input.shape[0]
    model_width = later_input.shape[1]
    hidden_units = up_weight.shape[1]
    seq_len = tokens_all // N_FS
    block_cols = hidden_units // N_TP
    grad_scale = jnp.float32(tokens_all ** (-0.5))
    taps_up = up_taps.astype(jnp.float32)
    taps_gate = gate_taps.astype(jnp.float32)

    def group(carry, inputs):
        sum_up, sum_gate, sum_taps_up, sum_taps_gate = carry
        later_rows, saved_rows, upstream = inputs
        up_later = jnp.dot(later_rows, up_weight, preferred_element_type=jnp.float32).astype(jnp.bfloat16)
        gate_later = jnp.dot(later_rows, gate_weight, preferred_element_type=jnp.float32).astype(jnp.bfloat16)
        conv_up = depthwise(up_later.astype(jnp.float32), taps_up)
        conv_gate = depthwise(gate_later.astype(jnp.float32), taps_gate)
        hidden_rows = (jax.nn.silu(conv_gate) * conv_up).astype(jnp.bfloat16)
        up_saved = jnp.dot(saved_rows, up_weight, preferred_element_type=jnp.float32).astype(jnp.bfloat16)
        gate_saved = jnp.dot(saved_rows, gate_weight, preferred_element_type=jnp.float32).astype(jnp.bfloat16)
        up_saved32 = up_saved.astype(jnp.float32)
        gate_saved32 = gate_saved.astype(jnp.float32)
        saved_up = depthwise(up_saved32, taps_up)
        saved_gate = depthwise(gate_saved32, taps_gate)
        sigmoid_gate = jax.nn.sigmoid(saved_gate)
        upstream32 = upstream.astype(jnp.float32)
        grad_conv_up = upstream32 * jax.nn.silu(saved_gate)
        grad_conv_gate = upstream32 * saved_up * sigmoid_gate * (1.0 + saved_gate * (1.0 - sigmoid_gate))
        grad_up = depthwise_back(grad_conv_up, taps_up).astype(jnp.bfloat16)
        grad_gate = depthwise_back(grad_conv_gate, taps_gate).astype(jnp.bfloat16)
        total = jnp.zeros((seq_len, model_width), jnp.float32)
        for block in range(N_TP):
            lower = block * block_cols
            upper = lower + block_cols
            partial_sum = jnp.dot(grad_up[:, lower:upper], up_weight[:, lower:upper].T, preferred_element_type=jnp.float32)
            partial_sum = partial_sum + jnp.dot(grad_gate[:, lower:upper], gate_weight[:, lower:upper].T, preferred_element_type=jnp.float32)
            rounded = lax.optimization_barrier(partial_sum.astype(jnp.bfloat16))
            total = total + rounded.astype(jnp.float32)
        dims = (((0,), (0,)), ((), ()))
        sum_up = sum_up + lax.dot_general(saved_rows, grad_up, dims, preferred_element_type=jnp.float32)
        sum_gate = sum_gate + lax.dot_general(saved_rows, grad_gate, dims, preferred_element_type=jnp.float32)
        sum_taps_up = sum_taps_up + taps_grad(grad_conv_up, up_saved32)
        sum_taps_gate = sum_taps_gate + taps_grad(grad_conv_gate, gate_saved32)
        return ((sum_up, sum_gate, sum_taps_up, sum_taps_gate), (hidden_rows, total.astype(jnp.bfloat16)))
    init = (jnp.zeros(up_weight.shape, jnp.float32), jnp.zeros(gate_weight.shape, jnp.float32), jnp.zeros(up_taps.shape, jnp.float32), jnp.zeros(gate_taps.shape, jnp.float32))
    inputs = (later_input.reshape(N_FS, seq_len, model_width), saved_input.reshape(N_FS, seq_len, model_width), cotangent.reshape(N_FS, seq_len, hidden_units))
    sums, outputs = lax.scan(group, init, inputs)
    hidden = outputs[0].reshape(tokens_all, hidden_units)
    input_grad = outputs[1].reshape(tokens_all, model_width)
    new_up_sum = up_grad_sum + grad_scale * sums[0]
    new_gate_sum = gate_grad_sum + grad_scale * sums[1]
    new_up_taps_sum = up_taps_sum + grad_scale * sums[2]
    new_gate_taps_sum = gate_taps_sum + grad_scale * sums[3]
    return (hidden, input_grad, new_up_sum, new_gate_sum, new_up_taps_sum, new_gate_taps_sum)
```

```python
import jax
import jax.numpy as jnp
from jax import lax
from jax.experimental import pallas as pl
from jax.experimental.pallas import tpu as pltpu
from jax.sharding import Mesh
from jax.sharding import PartitionSpec as P


FS = ("z", "x")
TP = ("y", "c")
FS_TP = ("z", "x", "y", "c")
BF16 = jnp.bfloat16
F32 = jnp.float32
LANES = 128
CHUNK = 64
KERNEL_VMEM = 20 << 20


def shift(array, axis, steps):
    peers = lax.axis_size(axis)
    return lax.ppermute(array, axis, [(i, (i + steps) % peers) for i in range(peers)])


def swapped(array, axis):
    return lax.ppermute(array, axis, [(0, 1), (1, 0)])


def exchanged(tiles, axis):
    return lax.all_to_all(tiles, axis, 0, 0, tiled=True)


def from_all(array, axis):
    return exchanged(jnp.broadcast_to(array[None], (lax.axis_size(axis), *array.shape)), axis)


def tiles_kernel(up_ref, gate_ref, tiles_ref):
    cols = up_ref.shape[1]
    for peer in range(tiles_ref.shape[0]):
        tiles_ref[peer, :, :cols] = up_ref[...]
        tiles_ref[peer, :, cols:] = gate_ref[...]


def rows_kernel(saved_ref, later_ref, rows_ref):
    rows_ref[0] = saved_ref[...]
    rows_ref[1] = later_ref[...]


def packed(kernel, shape, *arrays):
    return pl.pallas_call(
        kernel,
        out_shape=jax.ShapeDtypeStruct(shape, BF16),
        compiler_params=pltpu.CompilerParams(vmem_limit_bytes=8 << 20),
    )(*arrays)


def gather_rows(rows):
    y = lax.axis_index("y")
    half = rows.shape[1] // 2
    from_low = shift(rows, "y", 1)
    from_high = shift(rows, "y", -1)
    far_top = shift(from_low[:, :half], "y", 1)
    far_low = shift(from_high[:, half:], "y", -1)

    def placed(i):
        own = jnp.zeros((4, *rows.shape[1:]), rows.dtype)

        def put_rows(whole, block, index, start=0):
            return lax.dynamic_update_slice(whole, block[i][None], (index % 4, start, 0))

        own = put_rows(own, rows, y)
        own = put_rows(own, from_low, y + 3)
        own = put_rows(own, from_high, y + 1)
        own = put_rows(own, far_top, y + 2)
        own = put_rows(own, far_low, y + 2, half)
        return own.reshape(-1, rows.shape[2])

    saved, later = placed(0), placed(1)
    return (saved, swapped(saved, "c")), (later, swapped(later, "c"))


def project_into(own_ref, other_ref, up_ref, gate_ref, core_ref, values_ref):
    values_ref[:8, :] = jnp.zeros((8, values_ref.shape[1]), F32)
    weight = jnp.concatenate([up_ref[...], gate_ref[...]], axis=1)
    block = own_ref.shape[0] // 4
    for rows_ref, core in ((own_ref, core_ref[0]), (other_ref, 1 - core_ref[0])):
        part = jnp.dot(rows_ref[...], weight, preferred_element_type=F32)
        part = part.astype(BF16).astype(F32)
        for y in range(4):
            at = pl.multiple_of(8 + y * 2 * block + core * block, 8)
            values_ref[pl.ds(at, block), :] = part[y * block : (y + 1) * block]


def convolved(values, taps_ref):
    one, two, zero = pltpu.roll(values, 1, 0)[8:], pltpu.roll(values, 2, 0)[8:], values[8:]
    out = taps_ref[2:3, :] * zero + taps_ref[1:2, :] * one + taps_ref[0:1, :] * two
    return [two, one, zero], out


def hidden_kernel(
    core_ref, own_ref, other_ref, up_ref, gate_ref, taps_up_ref, taps_gate_ref, hidden_ref, values_ref
):
    project_into(own_ref, other_ref, up_ref, gate_ref, core_ref, values_ref)

    def step(i, carry):
        at = pl.multiple_of(i * CHUNK, CHUNK)
        up = convolved(values_ref[pl.ds(at, CHUNK + 8), :LANES], taps_up_ref)[1]
        gate = convolved(values_ref[pl.ds(at, CHUNK + 8), LANES:], taps_gate_ref)[1]
        hidden_ref[pl.ds(at, CHUNK), :] = (gate / (1.0 + jnp.exp(-gate)) * up).astype(BF16)
        return carry

    lax.fori_loop(0, hidden_ref.shape[0] // CHUNK, step, 0)


def grads_kernel(
    core_ref,
    own_ref,
    other_ref,
    up_ref,
    gate_ref,
    taps_up_ref,
    taps_gate_ref,
    cotangent_ref,
    grads_ref,
    sums_ref,
    values_ref,
    conv_ref,
):
    project_into(own_ref, other_ref, up_ref, gate_ref, core_ref, values_ref)
    tokens = 2 * own_ref.shape[0]
    count = tokens // CHUNK
    conv_ref[pl.ds(tokens, 8), :] = jnp.zeros((8, conv_ref.shape[1]), F32)
    lanes = [
        pl.ds(pl.multiple_of(pl.program_id(0) * LANES + part * (grads_ref.shape[1] // 2), LANES), LANES)
        for part in range(2)
    ]

    def step(i, sums):
        at = pl.multiple_of(i * CHUNK, CHUNK)
        ups, up = convolved(values_ref[pl.ds(at, CHUNK + 8), :LANES], taps_up_ref)
        gates, gate = convolved(
            values_ref[pl.ds(at, CHUNK + 8), LANES:], taps_gate_ref
        )
        sig = 1.0 / (1.0 + jnp.exp(-gate))
        upstream = cotangent_ref[pl.ds(at, CHUNK), :].astype(F32)
        grad_up = upstream * (gate * sig)
        grad_gate = upstream * up * sig * (1.0 + gate * (1.0 - sig))
        conv_ref[pl.ds(at, CHUNK), :LANES] = grad_up
        conv_ref[pl.ds(at, CHUNK), LANES:] = grad_gate

        def folded(values):
            return jnp.sum(values.reshape(CHUNK // 8, 8, LANES), axis=0)

        new = [folded(grad_up * v) for v in ups] + [folded(grad_gate * v) for v in gates]
        return tuple(a + b for a, b in zip(sums, new))

    zero = jnp.zeros((8, LANES), F32)
    sums = lax.fori_loop(0, count, step, (zero,) * 6)
    for k in range(3):
        for part in range(2):
            sums_ref[k : k + 1, lanes[part]] = jnp.sum(
                sums[3 * part + k], axis=0, keepdims=True
            )

    block = tokens // 8
    per_block = block // CHUNK

    def back(i, carry):
        at = pl.multiple_of(i * CHUNK, CHUNK)
        size = CHUNK + 8
        b = i // per_block
        away = lax.rem(b + core_ref[0], 2)
        to = away * (4 * block) + (b // 2) * block + lax.rem(i, per_block) * CHUNK
        to = pl.ds(pl.multiple_of(to, CHUNK), CHUNK)
        for part, taps_ref in enumerate((taps_up_ref, taps_gate_ref)):
            g = conv_ref[pl.ds(at, size), part * LANES : (part + 1) * LANES]
            one = pltpu.roll(g, size - 1, 0)[:CHUNK]
            two = pltpu.roll(g, size - 2, 0)[:CHUNK]
            out = taps_ref[2:3, :] * g[:CHUNK] + taps_ref[1:2, :] * one + taps_ref[0:1, :] * two
            grads_ref[to, lanes[part]] = out.astype(BF16)
        return carry

    lax.fori_loop(0, count, back, 0)


def common_specs(weights):
    steps = weights.shape[1] // (2 * LANES)
    whole = pl.BlockSpec(memory_space=pltpu.VMEM)
    taps = pl.BlockSpec((3, LANES), lambda j: (0, j))
    return [
        pl.BlockSpec(memory_space=pltpu.SMEM),
        whole,
        whole,
        pl.BlockSpec((weights.shape[0], LANES), lambda j: (0, j)),
        pl.BlockSpec((weights.shape[0], LANES), lambda j: (0, j + steps)),
        taps,
        taps,
    ]


def hidden_of(core, own, other, weights, taps_up, taps_gate):
    tokens, steps = 2 * own.shape[0], weights.shape[1] // (2 * LANES)
    return pl.pallas_call(
        hidden_kernel,
        grid=(steps,),
        in_specs=common_specs(weights),
        out_specs=pl.BlockSpec((tokens, LANES), lambda j: (0, j)),
        out_shape=jax.ShapeDtypeStruct((tokens, steps * LANES), BF16),
        scratch_shapes=[pltpu.VMEM((tokens + 8, 2 * LANES), F32)],
        compiler_params=pltpu.CompilerParams(vmem_limit_bytes=KERNEL_VMEM),
        cost_estimate=pl.CostEstimate(
            flops=2 * tokens * weights.size, transcendentals=0, bytes_accessed=8 << 20
        ),
    )(core, own, other, weights, weights, taps_up, taps_gate)


def grads_of(core, own, other, weights, taps_up, taps_gate, cotangent):
    tokens, steps = 2 * own.shape[0], weights.shape[1] // (2 * LANES)
    return pl.pallas_call(
        grads_kernel,
        grid=(steps,),
        in_specs=common_specs(weights)
        + [pl.BlockSpec((tokens, LANES), lambda j: (0, j))],
        out_specs=[
            pl.BlockSpec((tokens, weights.shape[1]), lambda j: (0, 0)),
            pl.BlockSpec((3, weights.shape[1]), lambda j: (0, 0)),
        ],
        out_shape=[
            jax.ShapeDtypeStruct((tokens, weights.shape[1]), BF16),
            jax.ShapeDtypeStruct((3, weights.shape[1]), F32),
        ],
        scratch_shapes=[
            pltpu.VMEM((tokens + 8, 2 * LANES), F32),
            pltpu.VMEM((tokens + 8, 2 * LANES), F32),
        ],
        compiler_params=pltpu.CompilerParams(vmem_limit_bytes=KERNEL_VMEM),
        cost_estimate=pl.CostEstimate(
            flops=2 * tokens * weights.size, transcendentals=0, bytes_accessed=8 << 20
        ),
    )(core, own, other, weights, weights, taps_up, taps_gate, cotangent)


def sum_rows_to_owner(grads, weights):
    half = grads.shape[0] // 2

    def partial(rows):
        out = lax.dot_general(rows, weights, (((1,), (1,)), ((), ())), preferred_element_type=F32)
        return out.astype(BF16)

    arrived = swapped(partial(grads[half:]), "c")
    chunks = (partial(grads[:half]).astype(F32) + arrived.astype(F32)).astype(BF16)
    y = lax.axis_index("y")
    chunks = chunks.reshape(4, -1, chunks.shape[1])
    half = chunks.shape[1] // 2

    def take(step):
        return lax.dynamic_index_in_dim(chunks, (y + step) % 4, 0, keepdims=False)

    far = take(2)
    far_top = shift(far[:half], "y", 1).astype(F32)
    far_low = shift(far[half:], "y", -1).astype(F32)
    up, down = take(1).astype(F32), take(3).astype(F32)
    up = jnp.concatenate([up[:half] + far_top, up[half:]], axis=0).astype(BF16)
    down = jnp.concatenate([down[:half], down[half:] + far_low], axis=0).astype(BF16)
    from_low = shift(up, "y", 1).astype(F32)
    from_high = shift(down, "y", -1).astype(F32)
    return (take(0).astype(F32) + from_low + from_high).astype(BF16)


def sum_to_owner_x(block):
    tiles = block.reshape(4, -1, block.shape[1])
    return exchanged(tiles, "x").astype(F32).sum(axis=0)


def body(
    later_input,
    saved_input,
    cotangent,
    up_weight,
    gate_weight,
    up_taps,
    gate_taps,
    up_grad_sum,
    gate_grad_sum,
    up_taps_sum,
    gate_taps_sum,
):
    cols = up_weight.shape[1]
    group = lax.axis_size(TP)
    offset = lax.axis_index(TP) * cols
    tokens = later_input.shape[0] * lax.axis_size(FS) * group
    grad_scale = jnp.float32(tokens ** (-0.5))
    taps_up = lax.dynamic_slice_in_dim(up_taps, offset, cols, 1).astype(F32)
    taps_gate = lax.dynamic_slice_in_dim(gate_taps, offset, cols, 1).astype(F32)
    core = jnp.full((1,), lax.axis_index("c"), jnp.int32)

    tiles = packed(tiles_kernel, (4, up_weight.shape[0], 2 * cols), up_weight, gate_weight)
    rows = packed(rows_kernel, (2, *saved_input.shape), saved_input, later_input)
    near = exchanged(tiles, "x").reshape(-1, 2 * cols)
    weights = lax.all_gather(near, "z", axis=0, tiled=True)
    saved, later = gather_rows(rows)

    both = jnp.concatenate(saved, axis=0)
    both, saved, later = lax.optimization_barrier((both, saved, later))
    grads, taps_local = grads_of(core, *saved, weights, taps_up, taps_gate, cotangent)
    term = lax.dot_general(
        both, grads, (((0,), (0,)), ((), ())), preferred_element_type=F32
    ).astype(BF16)
    own_z = lax.psum_scatter(term, "z", scatter_dimension=0, tiled=True)

    input_grad = sum_rows_to_owner(grads, weights)
    hidden = hidden_of(core, *later, weights, taps_up, taps_gate)
    taps_z = from_all(taps_local, "z").sum(axis=0)
    taps_all = from_all(from_all(taps_z, TP), "x").sum(axis=0)

    own = sum_to_owner_x(own_z)
    taps_all = taps_all.reshape(group, 3, 2, cols).transpose(2, 1, 0, 3).reshape(2, 3, -1)
    return (
        hidden,
        input_grad,
        up_grad_sum + grad_scale * own[:, :cols],
        gate_grad_sum + grad_scale * own[:, cols:],
        up_taps_sum + grad_scale * taps_all[0],
        gate_taps_sum + grad_scale * taps_all[1],
    )


def solution(mesh):
    finer = Mesh(mesh.devices.reshape(8, 4, 4, 2), ("z", "x", "y", "c"))
    in_specs = (
        P(FS_TP, None),
        P(FS_TP, None),
        P(FS, TP),
        P(FS, TP),
        P(FS, TP),
        P(),
        P(),
        P(FS, TP),
        P(FS, TP),
        P(),
        P(),
    )
    out_specs = (P(FS, TP), P(FS_TP, None), P(FS, TP), P(FS, TP), P(), P())
    return jax.shard_map(body, mesh=finer, in_specs=in_specs, out_specs=out_specs, check_vma=False)
```

```python
import jax
import jax.numpy as jnp
from jax import lax
from jax.experimental import pallas as pl
from jax.experimental.pallas import tpu as pltpu
from jax.sharding import Mesh
from jax.sharding import PartitionSpec as P


FS = ("z", "x")
TP = ("y", "c")
FS_TP = ("z", "x", "y", "c")
BF16 = jnp.bfloat16
F32 = jnp.float32
LANES = 128
CHUNK = 64
KERNEL_VMEM = 20 << 20


def shift(array, axis, steps):
    peers = lax.axis_size(axis)
    return lax.ppermute(array, axis, [(i, (i + steps) % peers) for i in range(peers)])


def swapped(array, axis):
    return lax.ppermute(array, axis, [(0, 1), (1, 0)])


def exchanged(tiles, axis):
    return lax.all_to_all(tiles, axis, 0, 0, tiled=True)


def from_all(array, axis):
    return exchanged(jnp.broadcast_to(array[None], (lax.axis_size(axis), *array.shape)), axis)


def tiles_kernel(up_ref, gate_ref, tiles_ref):
    cols = up_ref.shape[1]
    for peer in range(tiles_ref.shape[0]):
        tiles_ref[peer, :, :cols] = up_ref[...]
        tiles_ref[peer, :, cols:] = gate_ref[...]


def rows_kernel(saved_ref, later_ref, rows_ref):
    rows_ref[0] = saved_ref[...]
    rows_ref[1] = later_ref[...]


def packed(kernel, shape, *arrays):
    return pl.pallas_call(
        kernel,
        out_shape=jax.ShapeDtypeStruct(shape, BF16),
        compiler_params=pltpu.CompilerParams(vmem_limit_bytes=8 << 20),
    )(*arrays)


def gather_rows(rows):
    y = lax.axis_index("y")
    half = rows.shape[1] // 2
    from_low = shift(rows, "y", 1)
    from_high = shift(rows, "y", -1)
    far_top = shift(from_low[:, :half], "y", 1)
    far_low = shift(from_high[:, half:], "y", -1)

    def placed(i):
        own = jnp.zeros((4, *rows.shape[1:]), rows.dtype)

        def put_rows(whole, block, index, start=0):
            return lax.dynamic_update_slice(whole, block[i][None], (index % 4, start, 0))

        own = put_rows(own, rows, y)
        own = put_rows(own, from_low, y + 3)
        own = put_rows(own, from_high, y + 1)
        own = put_rows(own, far_top, y + 2)
        own = put_rows(own, far_low, y + 2, half)
        return own.reshape(-1, rows.shape[2])

    saved, later = placed(0), placed(1)
    return (saved, swapped(saved, "c")), (later, swapped(later, "c"))


def project_into(own_ref, other_ref, up_ref, gate_ref, core_ref, values_ref):
    values_ref[:8, :] = jnp.zeros((8, values_ref.shape[1]), F32)
    weight = jnp.concatenate([up_ref[...], gate_ref[...]], axis=1)
    block = own_ref.shape[0] // 4
    for rows_ref, core in ((own_ref, core_ref[0]), (other_ref, 1 - core_ref[0])):
        part = jnp.dot(rows_ref[...], weight, preferred_element_type=F32)
        part = part.astype(BF16).astype(F32)
        for y in range(4):
            at = pl.multiple_of(8 + y * 2 * block + core * block, 8)
            values_ref[pl.ds(at, block), :] = part[y * block : (y + 1) * block]


def convolved(values, taps_ref):
    one, two, zero = pltpu.roll(values, 1, 0)[8:], pltpu.roll(values, 2, 0)[8:], values[8:]
    out = taps_ref[2:3, :] * zero + taps_ref[1:2, :] * one + taps_ref[0:1, :] * two
    return [two, one, zero], out


def hidden_kernel(
    core_ref, own_ref, other_ref, up_ref, gate_ref, taps_up_ref, taps_gate_ref, hidden_ref, values_ref
):
    project_into(own_ref, other_ref, up_ref, gate_ref, core_ref, values_ref)

    def step(i, carry):
        at = pl.multiple_of(i * CHUNK, CHUNK)
        up = convolved(values_ref[pl.ds(at, CHUNK + 8), :LANES], taps_up_ref)[1]
        gate = convolved(values_ref[pl.ds(at, CHUNK + 8), LANES:], taps_gate_ref)[1]
        hidden_ref[pl.ds(at, CHUNK), :] = (gate / (1.0 + jnp.exp(-gate)) * up).astype(BF16)
        return carry

    lax.fori_loop(0, hidden_ref.shape[0] // CHUNK, step, 0)


def grads_kernel(
    core_ref,
    own_ref,
    other_ref,
    up_ref,
    gate_ref,
    taps_up_ref,
    taps_gate_ref,
    cotangent_ref,
    grads_ref,
    sums_ref,
    values_ref,
    conv_ref,
):
    project_into(own_ref, other_ref, up_ref, gate_ref, core_ref, values_ref)
    tokens = 2 * own_ref.shape[0]
    count = tokens // CHUNK
    conv_ref[pl.ds(tokens, 8), :] = jnp.zeros((8, conv_ref.shape[1]), F32)
    lanes = [
        pl.ds(pl.multiple_of(pl.program_id(0) * LANES + part * (grads_ref.shape[1] // 2), LANES), LANES)
        for part in range(2)
    ]

    def step(i, sums):
        at = pl.multiple_of(i * CHUNK, CHUNK)
        ups, up = convolved(values_ref[pl.ds(at, CHUNK + 8), :LANES], taps_up_ref)
        gates, gate = convolved(
            values_ref[pl.ds(at, CHUNK + 8), LANES:], taps_gate_ref
        )
        sig = 1.0 / (1.0 + jnp.exp(-gate))
        upstream = cotangent_ref[pl.ds(at, CHUNK), :].astype(F32)
        grad_up = upstream * (gate * sig)
        grad_gate = upstream * up * sig * (1.0 + gate * (1.0 - sig))
        conv_ref[pl.ds(at, CHUNK), :LANES] = grad_up
        conv_ref[pl.ds(at, CHUNK), LANES:] = grad_gate

        def folded(values):
            return jnp.sum(values.reshape(CHUNK // 8, 8, LANES), axis=0)

        new = [folded(grad_up * v) for v in ups] + [folded(grad_gate * v) for v in gates]
        return tuple(a + b for a, b in zip(sums, new))

    zero = jnp.zeros((8, LANES), F32)
    sums = lax.fori_loop(0, count, step, (zero,) * 6)
    for k in range(3):
        for part in range(2):
            sums_ref[k : k + 1, lanes[part]] = jnp.sum(
                sums[3 * part + k], axis=0, keepdims=True
            )

    block = tokens // 8
    per_block = block // CHUNK

    def back(i, carry):
        at = pl.multiple_of(i * CHUNK, CHUNK)
        size = CHUNK + 8
        b = i // per_block
        away = lax.rem(b + core_ref[0], 2)
        to = away * (4 * block) + (b // 2) * block + lax.rem(i, per_block) * CHUNK
        to = pl.ds(pl.multiple_of(to, CHUNK), CHUNK)
        for part, taps_ref in enumerate((taps_up_ref, taps_gate_ref)):
            g = conv_ref[pl.ds(at, size), part * LANES : (part + 1) * LANES]
            one = pltpu.roll(g, size - 1, 0)[:CHUNK]
            two = pltpu.roll(g, size - 2, 0)[:CHUNK]
            out = taps_ref[2:3, :] * g[:CHUNK] + taps_ref[1:2, :] * one + taps_ref[0:1, :] * two
            grads_ref[to, lanes[part]] = out.astype(BF16)
        return carry

    lax.fori_loop(0, count, back, 0)


def common_specs(weights):
    steps = weights.shape[1] // (2 * LANES)
    whole = pl.BlockSpec(memory_space=pltpu.VMEM)
    taps = pl.BlockSpec((3, LANES), lambda j: (0, j))
    return [
        pl.BlockSpec(memory_space=pltpu.SMEM),
        whole,
        whole,
        pl.BlockSpec((weights.shape[0], LANES), lambda j: (0, j)),
        pl.BlockSpec((weights.shape[0], LANES), lambda j: (0, j + steps)),
        taps,
        taps,
    ]


def hidden_of(core, own, other, weights, taps_up, taps_gate):
    tokens, steps = 2 * own.shape[0], weights.shape[1] // (2 * LANES)
    return pl.pallas_call(
        hidden_kernel,
        grid=(steps,),
        in_specs=common_specs(weights),
        out_specs=pl.BlockSpec((tokens, LANES), lambda j: (0, j)),
        out_shape=jax.ShapeDtypeStruct((tokens, steps * LANES), BF16),
        scratch_shapes=[pltpu.VMEM((tokens + 8, 2 * LANES), F32)],
        compiler_params=pltpu.CompilerParams(vmem_limit_bytes=KERNEL_VMEM),
        cost_estimate=pl.CostEstimate(
            flops=2 * tokens * weights.size, transcendentals=0, bytes_accessed=8 << 20
        ),
    )(core, own, other, weights, weights, taps_up, taps_gate)


def grads_of(core, own, other, weights, taps_up, taps_gate, cotangent):
    tokens, steps = 2 * own.shape[0], weights.shape[1] // (2 * LANES)
    return pl.pallas_call(
        grads_kernel,
        grid=(steps,),
        in_specs=common_specs(weights)
        + [pl.BlockSpec((tokens, LANES), lambda j: (0, j))],
        out_specs=[
            pl.BlockSpec((tokens, weights.shape[1]), lambda j: (0, 0)),
            pl.BlockSpec((3, weights.shape[1]), lambda j: (0, 0)),
        ],
        out_shape=[
            jax.ShapeDtypeStruct((tokens, weights.shape[1]), BF16),
            jax.ShapeDtypeStruct((3, weights.shape[1]), F32),
        ],
        scratch_shapes=[
            pltpu.VMEM((tokens + 8, 2 * LANES), F32),
            pltpu.VMEM((tokens + 8, 2 * LANES), F32),
        ],
        compiler_params=pltpu.CompilerParams(vmem_limit_bytes=KERNEL_VMEM),
        cost_estimate=pl.CostEstimate(
            flops=2 * tokens * weights.size, transcendentals=0, bytes_accessed=8 << 20
        ),
    )(core, own, other, weights, weights, taps_up, taps_gate, cotangent)


def sum_rows_to_owner(grads, weights):
    half = grads.shape[0] // 2

    def partial(rows):
        out = lax.dot_general(rows, weights, (((1,), (1,)), ((), ())), preferred_element_type=F32)
        return out.astype(BF16)

    arrived = swapped(partial(grads[half:]), "c")
    chunks = (partial(grads[:half]).astype(F32) + arrived.astype(F32)).astype(BF16)
    y = lax.axis_index("y")
    chunks = chunks.reshape(4, -1, chunks.shape[1])
    half = chunks.shape[1] // 2

    def take(step):
        return lax.dynamic_index_in_dim(chunks, (y + step) % 4, 0, keepdims=False)

    far = take(2)
    far_top = shift(far[:half], "y", 1).astype(F32)
    far_low = shift(far[half:], "y", -1).astype(F32)
    up, down = take(1).astype(F32), take(3).astype(F32)
    up = jnp.concatenate([up[:half] + far_top, up[half:]], axis=0).astype(BF16)
    down = jnp.concatenate([down[:half], down[half:] + far_low], axis=0).astype(BF16)
    from_low = shift(up, "y", 1).astype(F32)
    from_high = shift(down, "y", -1).astype(F32)
    return (take(0).astype(F32) + from_low + from_high).astype(BF16)


def sum_to_owner_x(block):
    tiles = block.reshape(4, -1, block.shape[1])
    return exchanged(tiles, "x").astype(F32).sum(axis=0)


def body(
    later_input,
    saved_input,
    cotangent,
    up_weight,
    gate_weight,
    up_taps,
    gate_taps,
    up_grad_sum,
    gate_grad_sum,
    up_taps_sum,
    gate_taps_sum,
):
    cols = up_weight.shape[1]
    group = lax.axis_size(TP)
    offset = lax.axis_index(TP) * cols
    tokens = later_input.shape[0] * lax.axis_size(FS) * group
    grad_scale = jnp.float32(tokens ** (-0.5))
    taps_up = lax.dynamic_slice_in_dim(up_taps, offset, cols, 1).astype(F32)
    taps_gate = lax.dynamic_slice_in_dim(gate_taps, offset, cols, 1).astype(F32)
    core = jnp.full((1,), lax.axis_index("c"), jnp.int32)

    tiles = packed(tiles_kernel, (4, up_weight.shape[0], 2 * cols), up_weight, gate_weight)
    rows = packed(rows_kernel, (2, *saved_input.shape), saved_input, later_input)
    near = exchanged(tiles, "x").reshape(-1, 2 * cols)
    weights = lax.all_gather(near, "z", axis=0, tiled=True)
    saved, later = gather_rows(rows)

    both = jnp.concatenate(saved, axis=0)
    both, saved, later = lax.optimization_barrier((both, saved, later))
    grads, taps_local = grads_of(core, *saved, weights, taps_up, taps_gate, cotangent)
    term = lax.dot_general(
        both, grads, (((0,), (0,)), ((), ())), preferred_element_type=F32
    ).astype(BF16)
    own_z = lax.psum_scatter(term, "z", scatter_dimension=0, tiled=True)

    input_grad = sum_rows_to_owner(grads, weights)
    hidden = hidden_of(core, *later, weights, taps_up, taps_gate)
    taps_z = from_all(taps_local, "z").sum(axis=0)
    taps_all = from_all(from_all(taps_z, TP), "x").sum(axis=0)

    own = sum_to_owner_x(own_z)
    taps_all = taps_all.reshape(group, 3, 2, cols).transpose(2, 1, 0, 3).reshape(2, 3, -1)
    new_up_taps = up_taps_sum + grad_scale * taps_all[0]
    new_gate_taps = gate_taps_sum + grad_scale * taps_all[1]
    return (
        hidden,
        input_grad,
        up_grad_sum + grad_scale * own[:, :cols],
        gate_grad_sum + grad_scale * own[:, cols:],
        new_up_taps,
        new_gate_taps,
    )


def solution(mesh):
    finer = Mesh(mesh.devices.reshape(8, 4, 4, 2), ("z", "x", "y", "c"))
    in_specs = (
        P(FS_TP, None),
        P(FS_TP, None),
        P(FS, TP),
        P(FS, TP),
        P(FS, TP),
        P(),
        P(),
        P(FS, TP),
        P(FS, TP),
        P(),
        P(),
    )
    out_specs = (P(FS, TP), P(FS_TP, None), P(FS, TP), P(FS, TP), P(), P())
    return jax.shard_map(body, mesh=finer, in_specs=in_specs, out_specs=out_specs, check_vma=False)
```
